32 devices in a mesh: grp: 2 (over y), kv: 4 (over z), tp: 4 (over x, core).
Axes of the slice: x: 2, y: 2, z: 4, core: 2. Of those that a mesh axis runs over, the one named last changes fastest.
Arguments:
- residual: bfloat16 [32, 4096], P('grp', ('kv', 'tp')), parts along dimension 0, may hold values from -11 to 11
- cache_keys: bfloat16 [32, 4096, 8, 128], P('grp', 'kv', 'tp'), parts along dimension 0, may hold values from -210 to 210
- cache_values: bfloat16 [32, 4096, 8, 128], P('grp', 'kv', 'tp'), parts along dimension 0, may hold values from -6 to 6
- norm_gain: bfloat16 [4096], P('kv'), may hold values from 0.099609375 to 1.8984375
- query_weight: bfloat16 [4096, 2048], P('kv', 'tp'), may hold values from -0.09375 to 0.09375
- key_weight: bfloat16 [4096, 1024], P('kv', 'tp'), may hold values from -0.25 to 0.25
- value_weight: bfloat16 [4096, 1024], P('kv', 'tp'), may hold values from -0.375 to 0.375
- head_lambda: float32 [16], P('tp'), may hold values from 0.3 to 0.8
- head_gain: bfloat16 [128], replicated, may hold values from 0.099609375 to 1.8984375
- out_weight: bfloat16 [2048, 4096], P('tp', 'kv'), may hold values from -0.1875 to 0.1875
- mixer_gain: bfloat16 [4096], P('kv'), may hold values from 0.099609375 to 1.8984375
- up_weight: bfloat16 [4096, 16384], P('kv', 'tp'), may hold values from -0.09375 to 0.09375
- down_weight: bfloat16 [16384, 4096], P('tp', 'kv'), may hold values from -0.0625 to 0.0625
Outputs:
- updated: bfloat16 [32, 4096], P('grp', ('kv', 'tp')), parts along dimension 0
The draws below stay inside these ranges and needn't reach their ends.
There are 2 independent parts, one for each index of `grp`. The reference program is written for one: setup_inputs(seed, part) draws one part's arguments, and reference() takes and returns one part's arrays. A program takes and returns all parts, laid end to end along the dimension named above; an argument that names none is the same for every part. Nothing has to cross between parts.
All inputs are finite; a program needn't handle non-finite values.
Results may differ from the reference program's by a relative error of at most 0.018.
Values may be sent and summed in bfloat16 or wider, within the bound.
A program may use at most 128 MiB of HBM per device.

```python
import jax
import jax.numpy as jnp
from jax import lax

D = 4096
HEADS = 16
KV_HEADS = 8
HALF = 64
VDIM = 128
FF = 16384
BATCH = 16
CTX = 4096


def draw_residual(key, part):
    first, second = jax.random.split(key, 2)
    column = jnp.arange(D, dtype=jnp.float32)
    rough = jax.random.uniform(first, (D,), jnp.float32, 0.5, 1.5)
    scale = 0.15 * 8.0 ** (column / D) * rough
    base = jnp.clip(jax.random.normal(second, (BATCH, D), jnp.float32), -6.0, 6.0)
    return (base * scale).astype(jnp.bfloat16)


def draw_cache_keys(key, part):
    first = jax.random.fold_in(key, 0)
    base = 1.75 * jnp.clip(jax.random.normal(first, (BATCH, CTX, KV_HEADS, 2 * HALF), jnp.float32), -6.0, 6.0)
    return base.astype(jnp.bfloat16)


def raised(result, key, source, target, blocks, factor):
    owner, partner = [(jnp.arange(result.shape[dim]) // (result.shape[dim] // blocks)).reshape([-1 if axis == dim else 1 for axis in range(result.ndim)]) for dim in (source, target)]
    chosen = jax.random.permutation(key, blocks)[partner]
    strong = (owner == chosen) | (owner == (partner + blocks // 2) % blocks)
    return jnp.where(strong, factor * result, result)


def levels(key, extent, shards, smallest, largest):
    def one(dim, blocks):
        draws = jax.random.uniform(jax.random.fold_in(jax.random.fold_in(key, 6), dim), (blocks,), jnp.float32, smallest / len(shards), largest / len(shards))
        return jnp.repeat(jnp.exp(draws), extent[dim] // blocks).reshape((-1,) + (1,) * (len(extent) - dim - 1))

    loudness = one(*shards[0])
    for cut in shards[1:]:
        loudness = loudness * one(*cut)
    return loudness


def normal_values(key, extent, deviation, most, shards=(), held_as=jnp.bfloat16):
    drawn = jax.random.normal(key, extent, jnp.float32) * deviation
    if len(shards) > 0:
        drawn = levels(key, extent, shards, -0.22, 0.18) * drawn
    return jnp.clip(drawn, min=-most, max=most).astype(held_as)


def bell_draw_with(own_key, dims, scale, most, cuts, heavy, kind=jnp.bfloat16):
    values = scale * jax.random.normal(own_key, dims, jnp.float32)
    if cuts:
        values = values * levels(own_key, dims, cuts, -0.22, 0.18)
    return jnp.clip(raised(values, jax.random.fold_in(own_key, 3), *heavy), -most, most).astype(kind)


def setup_inputs(seed: int = 0, part: int = 0) -> dict:
    streams_of = jax.random.split(jax.random.key(seed), 14)
    own_keys = jax.random.split(jax.random.fold_in(streams_of[13], part), 14)
    return {
        "residual": draw_residual(jax.random.fold_in(jax.random.fold_in(streams_of[13], part), 71), part),
        "cache_keys": draw_cache_keys(jax.random.fold_in(jax.random.fold_in(streams_of[13], part), 71), part),
        "cache_values": normal_values(own_keys[2], (BATCH, CTX, KV_HEADS, VDIM), 1.0, 6.0, ((1, 4), (2, 4))),
        "norm_gain": jnp.clip(1.0 + 0.18 * jax.random.normal(streams_of[3], (D,), jnp.float32), 0.099609375, 1.8984375).astype(jnp.bfloat16),
        "query_weight": normal_values(streams_of[4], (D, HEADS * 2 * HALF), D ** -0.5, 0.09375, ((0, 4), (1, 4))),
        "key_weight": normal_values(streams_of[5], (D, KV_HEADS * 2 * HALF), (D // 9) ** -0.5, 0.25, ((0, 4), (1, 4))),
        "value_weight": normal_values(streams_of[6], (D, KV_HEADS * VDIM), (D // 16) ** -0.5, 0.375, ((0, 4), (1, 4))),
        "head_lambda": jnp.clip(0.3 + 0.5 * jax.random.uniform(streams_of[7], (HEADS,), jnp.float32) ** levels(streams_of[7], (HEADS,), ((0, 4),), -0.2, 0.2), 0.3, 0.8),
        "head_gain": jnp.clip(1.0 + 0.18 * jax.random.normal(streams_of[8], (VDIM,), jnp.float32), 0.099609375, 1.8984375).astype(jnp.bfloat16),
        "out_weight": bell_draw_with(streams_of[9], (HEADS * VDIM, D), (HEADS * VDIM) ** -0.5, 0.1875, ((0, 4), (1, 4)), (0, 1, 4, 2.0)),
        "mixer_gain": jnp.clip(1.0 + 0.18 * jax.random.normal(streams_of[10], (D,), jnp.float32), 0.099609375, 1.8984375).astype(jnp.bfloat16),
        "up_weight": normal_values(streams_of[11], (D, FF), D ** -0.5, 0.09375, ((0, 4), (1, 4))),
        "down_weight": bell_draw_with(streams_of[12], (FF, D), FF ** -0.5, 0.0625, ((0, 4), (1, 4)), (0, 1, 4, 2.0)),
    }


EPS = 1e-06

def reference(residual, cache_keys, cache_values, norm_gain, query_weight, key_weight, value_weight, head_lambda, head_gain, out_weight, mixer_gain, up_weight, down_weight):
    f32 = jnp.float32
    bf16 = jnp.bfloat16
    group = HEADS // KV_HEADS
    scale = 1.0 / HALF ** 0.5
    resid = residual.astype(f32)
    scaled = (resid * norm_gain.astype(f32)).astype(bf16)
    inv_rms = lax.rsqrt(lax.optimization_barrier(jnp.mean(resid * resid, axis=1, keepdims=True)) + EPS)
    query = (inv_rms * jnp.dot(scaled, query_weight, preferred_element_type=f32)).astype(bf16)
    new_key = (inv_rms * jnp.dot(scaled, key_weight, preferred_element_type=f32)).astype(bf16)
    new_value = (inv_rms * jnp.dot(scaled, value_weight, preferred_element_type=f32)).astype(bf16)
    query = jnp.moveaxis(query.reshape(BATCH, KV_HEADS, group, 2, HALF), 1, 0)
    new_key = jnp.moveaxis(new_key.reshape(BATCH, KV_HEADS, 2, HALF), 1, 0)
    new_value = jnp.moveaxis(new_value.reshape(BATCH, KV_HEADS, VDIM), 1, 0)

    def one_head(args):
        q_head, k_own, v_own, index = args
        keys = lax.dynamic_index_in_dim(cache_keys, index, 2, keepdims=False).reshape(BATCH, CTX, 2, HALF)
        values = lax.dynamic_index_in_dim(cache_values, index, 2, keepdims=False)
        scores = jnp.einsum('bgch,bpch->bgcp', q_head.astype(f32), keys.astype(f32)) * scale
        cache_top = lax.optimization_barrier(jnp.max(scores, axis=3))
        expo = jnp.exp(scores - cache_top[..., None])
        total = lax.optimization_barrier(jnp.sum(expo, axis=3))
        probs = expo.astype(bf16)
        weighted = jnp.einsum('bgcp,bpv->bgcv', probs.astype(f32), values.astype(f32))
        own = jnp.einsum('bgch,bch->bgc', q_head.astype(f32), k_own.astype(f32)) * scale
        top = jnp.maximum(cache_top, own)
        old_part = jnp.exp(cache_top - top)
        own_part = jnp.exp(own - top)
        numer = weighted * old_part[..., None] + own_part[..., None] * v_own.astype(f32)[:, None, None, :]
        return numer / (total * old_part + own_part)[..., None]
    attended = lax.map(one_head, (query, new_key, new_value, jnp.arange(KV_HEADS, dtype=jnp.int32)))
    attended = jnp.moveaxis(attended, 0, 1).reshape(BATCH, HEADS, 2, VDIM)
    diff = attended[:, :, 0] - head_lambda[None, :, None] * attended[:, :, 1]
    normed = diff * lax.rsqrt(lax.optimization_barrier(jnp.mean(diff * diff, axis=2, keepdims=True)) + EPS) * head_gain.astype(f32)
    heads_out = normed.astype(bf16).reshape(BATCH, HEADS * VDIM)
    mixed = (resid + jnp.dot(heads_out, out_weight, preferred_element_type=f32)).astype(bf16)
    mixed_f = mixed.astype(f32)
    scaled2 = (mixed_f * mixer_gain.astype(f32)).astype(bf16)
    inv_rms2 = lax.rsqrt(lax.optimization_barrier(jnp.mean(mixed_f * mixed_f, axis=1, keepdims=True)) + EPS)
    up = inv_rms2 * jnp.dot(scaled2, up_weight, preferred_element_type=f32)
    hidden = jnp.square(jnp.maximum(up, 0.0)).astype(bf16)
    return (mixed_f + jnp.dot(hidden, down_weight, preferred_element_type=f32)).astype(bf16)
```

```python
import functools

import jax
import jax.numpy as jnp
from jax import lax
from jax.experimental import pallas as pl
from jax.experimental.pallas import tpu as pltpu
from jax.sharding import PartitionSpec as P

D = 4096
HEADS = 16
KV_HEADS = 8
HALF = 64
VDIM = 128


EPS = 1e-06


def joined(shard, axis, combine):
    everything = jax.tree.map(lambda part: lax.all_gather(part, axis), shard)
    first = jax.tree.map(lambda part: part[0], everything)

    def step(k, so_far):
        return combine(so_far, jax.tree.map(lambda part: part[k], everything))

    return lax.fori_loop(1, lax.axis_size(axis), step, first)


def combine(first, second):
    top = jnp.maximum(first[0], second[0])
    left = jnp.exp(first[0] - top)
    right = jnp.exp(second[0] - top)
    return (
        top,
        first[1] * left + second[1] * right,
        first[2] * left[..., None] + second[2] * right[..., None],
    )


def plain_body(
    residual,
    cache_keys,
    cache_values,
    norm_gain,
    query_weight,
    key_weight,
    value_weight,
    head_lambda,
    head_gain,
    out_weight,
    mixer_gain,
    up_weight,
    down_weight,
):
    f32 = jnp.float32
    bf16 = jnp.bfloat16
    rows = residual.shape[0]
    kv_local = cache_keys.shape[2]
    group = HEADS // KV_HEADS
    scale = 1.0 / HALF**0.5
    block = lax.all_gather(residual, "tp", axis=1, tiled=True).astype(f32)
    scaled = (block * norm_gain.astype(f32)).astype(bf16)
    q_part = jnp.dot(scaled, query_weight, preferred_element_type=f32)
    k_part = jnp.dot(scaled, key_weight, preferred_element_type=f32)
    v_part = jnp.dot(scaled, value_weight, preferred_element_type=f32)
    sq_part = jnp.sum(block * block, axis=1)
    q_sum, k_sum, v_sum, sq_sum = lax.psum((q_part, k_part, v_part, sq_part), "kv")
    inv_rms = lax.rsqrt(sq_sum / D + EPS)[:, None]
    query = (inv_rms * q_sum).astype(bf16).reshape(rows, kv_local, group, 2, HALF)
    new_key = (inv_rms * k_sum).astype(bf16).reshape(rows, kv_local, 2, HALF)
    new_value = (inv_rms * v_sum).astype(bf16).reshape(rows, kv_local, VDIM)
    positions = cache_keys.shape[1]
    keys = cache_keys.reshape(rows, positions, kv_local, 2, HALF)
    scores = jnp.einsum("bkgch,bpkch->bkgcp", query, keys, preferred_element_type=f32) * scale
    local_top = jnp.max(scores, axis=4)
    expo = jnp.exp(scores - local_top[..., None])
    local_total = jnp.sum(expo, axis=4)
    local_weighted = jnp.einsum(
        "bkgcp,bpkv->bkgcv", expo.astype(bf16), cache_values, preferred_element_type=f32
    )
    cache_top, total, weighted = joined((local_top, local_total, local_weighted), "kv", combine)
    own = jnp.einsum("bkgch,bkch->bkgc", query, new_key, preferred_element_type=f32) * scale
    top = jnp.maximum(cache_top, own)
    old_part = jnp.exp(cache_top - top)
    own_part = jnp.exp(own - top)
    numer = (
        weighted * old_part[..., None]
        + own_part[..., None] * new_value.astype(f32)[:, :, None, None, :]
    )
    attended = numer / (total * old_part + own_part)[..., None]
    lambdas = head_lambda.reshape(kv_local, group)[None, :, :, None]
    diff = attended[:, :, :, 0] - lambdas * attended[:, :, :, 1]
    normed = (
        diff * lax.rsqrt(jnp.mean(diff * diff, axis=3, keepdims=True) + EPS) * head_gain.astype(f32)
    )
    heads_out = normed.astype(bf16).reshape(rows, kv_local * group * VDIM)
    projected = jnp.dot(heads_out, out_weight, preferred_element_type=f32)
    mixed = (
        residual.astype(f32) + lax.psum_scatter(projected, "tp", scatter_dimension=1, tiled=True)
    ).astype(bf16)
    mixed_block = lax.all_gather(mixed, "tp", axis=1, tiled=True).astype(f32)
    scaled2 = (mixed_block * mixer_gain.astype(f32)).astype(bf16)
    up_part = jnp.dot(scaled2, up_weight, preferred_element_type=f32)
    sq_mixed = jnp.sum(mixed_block * mixed_block, axis=1)
    up_share = lax.psum_scatter(up_part, "kv", scatter_dimension=1, tiled=True)
    sq_total = lax.psum(sq_mixed, "kv")
    inv_rms2 = lax.rsqrt(sq_total / D + EPS)[:, None]
    share = jnp.square(jnp.maximum(inv_rms2 * up_share, 0.0)).astype(bf16)
    hidden = lax.all_gather(share, "kv", axis=1, tiled=True)
    down_part = jnp.dot(hidden, down_weight, preferred_element_type=f32)
    return (
        mixed.astype(f32) + lax.psum_scatter(down_part, "tp", scatter_dimension=1, tiled=True)
    ).astype(bf16)


def spread(column, lanes):
    high = column.astype(jnp.bfloat16).astype(jnp.float32)
    lane = lax.broadcasted_iota(jnp.int32, (column.shape[0], lanes), 1)
    return jnp.where(lane < lanes // 2, high, column - high).astype(jnp.bfloat16)


def gathered(pair):
    pair = pair.astype(jnp.float32)
    half = pair.shape[1] // 2
    return pair[:, 0:1] + pair[:, half : half + 1]


def layer_kernel(
    dims,
    residual_ref,
    gains_ref,
    lambda_ref,
    keys_hbm,
    values_hbm,
    qw_hbm,
    kw_hbm,
    vw_hbm,
    ow_hbm,
    uw_hbm,
    dw_hbm,
    out_ref,
    keys,
    values,
    qw,
    kw,
    vw,
    ow,
    uw,
    dw,
    x_all,
    q_send,
    q_recv,
    n_send,
    n_recv,
    q_rows,
    k_rows,
    v_rows,
    w_own,
    w_send,
    w_recv,
    s_send,
    s_recv,
    att,
    o_all,
    o_send,
    m_send,
    m_recv,
    u_send,
    u_recv,
    h_send,
    h_recv,
    d_send,
    d_recv,
    load_sem,
    cache_sem,
    x_sem,
    q_sem,
    n_sem,
    w_sem,
    s_sem,
    o_sem,
    m_sem,
    u_sem,
    h_sem,
    d_sem,
):
    f32 = jnp.float32
    bf16 = jnp.bfloat16
    kvn, tpn, kv_local, groups = dims
    rows = residual_ref.shape[0]
    width = residual_ref.shape[1]
    q_cols = qw.shape[1]
    k_cols = kw.shape[1]
    reps = q_cols // VDIM * 2
    per = rows // groups
    model = qw.shape[0] * kvn
    me_kv = lax.axis_index("kv")
    me_tp = lax.axis_index("tp")

    loads = []
    for index, (src, dst) in enumerate(((qw_hbm, qw), (kw_hbm, kw), (vw_hbm, vw))):
        loads.append(pltpu.make_async_copy(src, dst, load_sem.at[index]))
        loads[-1].start()

    def cache_copy(g, which):
        src, dst = ((keys_hbm, keys), (values_hbm, values))[which]
        span = pl.ds(g * per, per)
        return pltpu.make_async_copy(src.at[span], dst.at[span], cache_sem.at[g, which])

    for g in range(groups):
        cache_copy(g, 0).start()
        cache_copy(g, 1).start()
    for index, (src, dst) in enumerate(((ow_hbm, ow), (uw_hbm, uw), (dw_hbm, dw))):
        loads.append(pltpu.make_async_copy(src, dst, load_sem.at[3 + index]))
        loads[-1].start()

    def kv_to(d):
        return {"kv": lax.rem(me_kv + d, kvn)}

    def tp_to(d):
        return {"tp": lax.rem(me_tp + d, tpn)}

    def remote(src, dst, sems, index, target):
        return pltpu.make_async_remote_copy(
            src_ref=src,
            dst_ref=dst,
            send_sem=sems.at[(0,) + index],
            recv_sem=sems.at[(1,) + index],
            device_id=target,
            device_id_type=pl.DeviceIdType.MESH,
        )

    barrier = pltpu.get_barrier_semaphore()
    for d in range(1, tpn):
        pl.semaphore_signal(barrier, 1, device_id=tp_to(d), device_id_type=pl.DeviceIdType.MESH)
    for d in range(1, kvn):
        pl.semaphore_signal(barrier, 1, device_id=kv_to(d), device_id_type=pl.DeviceIdType.MESH)
    pl.semaphore_wait(barrier, tpn + kvn - 2)

    x_copies = [
        remote(residual_ref, x_all.at[me_tp], x_sem, (d,), tp_to(d)) for d in range(1, tpn)
    ]
    for copy in x_copies:
        copy.start()
    x_all[me_tp] = residual_ref[...]
    for copy in x_copies:
        copy.wait()

    block = jnp.concatenate([x_all[t] for t in range(tpn)], axis=1).astype(f32)
    scaled = (block * gains_ref[0:1, :]).astype(bf16)
    sq_own = jnp.sum(block * block, axis=1, keepdims=True)
    loads[0].wait()
    q_own = jnp.dot(scaled, qw[...], preferred_element_type=f32)
    q_send[:, 0:q_cols] = q_own.astype(bf16)
    q_send[:, q_cols:] = spread(sq_own, 128)
    q_copies = [remote(q_send, q_recv.at[d], q_sem, (d,), kv_to(d)) for d in range(1, kvn)]
    for copy in q_copies:
        copy.start()
    loads[1].wait()
    loads[2].wait()
    k_own = jnp.dot(scaled, kw[...], preferred_element_type=f32)
    v_own = jnp.dot(scaled, vw[...], preferred_element_type=f32)
    n_send[:, 0:k_cols] = k_own.astype(bf16)
    n_send[:, k_cols:] = v_own.astype(bf16)
    n_copies = [remote(n_send, n_recv.at[d], n_sem, (d,), kv_to(d)) for d in range(1, kvn)]
    for copy in n_copies:
        copy.start()
    for copy in q_copies:
        copy.wait()
    sq_sum = sq_own
    q_sum = q_own
    for d in range(1, kvn):
        sq_sum = sq_sum + gathered(q_recv[d, :, q_cols:])
        q_sum = q_sum + q_recv[d, :, 0:q_cols].astype(f32)
    inv_rms = lax.rsqrt(sq_sum / model + EPS)
    scale = 1.0 / HALF**0.5
    query = (inv_rms * q_sum).astype(bf16).astype(f32) * scale
    low_half = lax.broadcasted_iota(jnp.int32, (rows, VDIM), 1) < HALF
    for h in range(reps // 2):
        piece = query[:, h * VDIM : (h + 1) * VDIM]
        q_rows[:, 2 * h, :] = jnp.where(low_half, piece, 0.0)
        q_rows[:, 2 * h + 1, :] = jnp.where(low_half, 0.0, piece)

    columns = keys.shape[1]
    share = reps // kv_local
    col = lax.broadcasted_iota(jnp.int32, (reps, columns), 1)
    row = lax.broadcasted_iota(jnp.int32, (reps, columns), 0)
    valid = lax.rem(col, kv_local) == row // share
    lane = lax.broadcasted_iota(jnp.int32, (reps, 128), 1)

    def w_copy(g, d):
        span = pl.ds(pl.multiple_of(g * per * reps, per * reps), per * reps)
        return remote(w_send.at[span], w_recv.at[d, span], w_sem, (g, d), kv_to(d))

    def attend(g, stat):
        cache_copy(g, 0).wait()
        cache_copy(g, 1).wait()
        outs = []
        for i in range(per):
            b = g * per + i
            scores = lax.dot_general(
                q_rows[b].astype(bf16),
                keys[b],
                (((1,), (1,)), ((), ())),
                preferred_element_type=f32,
            )
            scores = jnp.where(valid, scores, -1e30)
            top = jnp.max(scores, axis=1, keepdims=True)
            expo = jnp.exp(scores - top)
            total = jnp.sum(expo, axis=1, keepdims=True)
            outs.append(jnp.dot(expo.astype(bf16), values[b], preferred_element_type=f32))
            stat = jnp.where(lane == b, top, stat)
            stat = jnp.where(lane == b + 64, total, stat)
        weighted = jnp.concatenate(outs, axis=0)
        span = pl.ds(pl.multiple_of(g * per * reps, per * reps), per * reps)
        w_own[span, :] = weighted
        w_send[span, :] = weighted.astype(bf16)
        for d in range(1, kvn):
            w_copy(g, d).start()
        return stat

    stat = lax.fori_loop(0, groups, attend, jnp.zeros((reps, 128), f32))
    s_send[...] = stat
    s_copies = [remote(s_send, s_recv.at[d], s_sem, (d,), kv_to(d)) for d in range(1, kvn)]
    for copy in s_copies:
        copy.start()

    for copy in n_copies:
        copy.wait()
    k_sum, v_sum = k_own, v_own
    for d in range(1, kvn):
        k_sum = k_sum + n_recv[d, :, 0:k_cols].astype(f32)
        v_sum = v_sum + n_recv[d, :, k_cols:].astype(f32)
    new_key = (inv_rms * k_sum).astype(bf16).astype(f32)
    new_value = (inv_rms * v_sum).astype(bf16).astype(f32)
    for r in range(reps):
        k = r // share
        k_rows[:, r, :] = new_key[:, k * VDIM : (k + 1) * VDIM]
        v_rows[:, r, :] = new_value[:, k * VDIM : (k + 1) * VDIM]
    own = jnp.zeros((reps, 128), f32)
    for b in range(rows):
        own = jnp.where(lane == b, jnp.sum(q_rows[b] * k_rows[b], axis=1, keepdims=True), own)

    for copy in s_copies:
        copy.wait()
    stats = [stat] + [s_recv[d] for d in range(1, kvn)]
    top = own
    for part in stats:
        top = jnp.maximum(top, part)
    own_part = jnp.exp(own - top)
    denom = own_part
    factors = []
    for part in stats:
        factors.append(jnp.exp(part - top))
        denom = denom + factors[-1] * pltpu.roll(part, 64, 1)
    own_part = own_part / denom
    factors = [factor / denom for factor in factors]
    for g in range(groups):
        for d in range(1, kvn):
            w_copy(g, d).wait()
    for b in range(rows):
        span = slice(b * reps, (b + 1) * reps)
        total = v_rows[b] * own_part[:, b : b + 1] + w_own[span, :] * factors[0][:, b : b + 1]
        for d in range(1, kvn):
            total = total + w_recv[d, span, :].astype(f32) * factors[d][:, b : b + 1]
        att[b] = total

    heads = []
    for h in range(reps // 2):
        diff = att[:, 2 * h, :] - lambda_ref[h] * att[:, 2 * h + 1, :]
        mean = jnp.mean(diff * diff, axis=1, keepdims=True)
        heads.append((diff * lax.rsqrt(mean + EPS) * gains_ref[2:3, 0:VDIM]).astype(bf16))
    heads_out = jnp.concatenate(heads, axis=1)
    loads[3].wait()
    o_send[...] = jnp.dot(heads_out, ow[...], preferred_element_type=f32).astype(bf16)
    o_copies = [remote(o_send, o_all.at[me_tp], o_sem, (d,), tp_to(d)) for d in range(1, tpn)]
    for copy in o_copies:
        copy.start()
    o_all[me_tp] = o_send[...]
    for copy in o_copies:
        copy.wait()
    mixed = o_all[0].astype(f32)
    for t in range(1, tpn):
        mixed = mixed + o_all[t].astype(f32)
    mixed = (block + mixed).astype(bf16).astype(f32)
    scaled2 = (mixed * gains_ref[1:2, :]).astype(bf16)
    sq_mixed = jnp.sum(mixed * mixed, axis=1, keepdims=True)
    m_send[...] = spread(sq_mixed, 128)
    m_copies = [remote(m_send, m_recv.at[d], m_sem, (d,), kv_to(d)) for d in range(1, kvn)]
    for copy in m_copies:
        copy.start()

    part = uw.shape[1] // kvn

    def up_for(j):
        span = pl.ds(pl.multiple_of(j * part, part), part)
        return jnp.dot(scaled2, uw[:, span], preferred_element_type=f32)

    loads[4].wait()
    u_copies = []
    for d in [kvn // 2] + [d for d in range(1, kvn) if d != kvn // 2]:
        u_send[d] = up_for(lax.rem(me_kv + d, kvn)).astype(bf16)
        u_copies.append(remote(u_send.at[d], u_recv.at[d], u_sem, (d,), kv_to(d)))
        u_copies[-1].start()
    up_sum = up_for(me_kv)
    for copy in m_copies:
        copy.wait()
    for d in range(1, kvn):
        sq_mixed = sq_mixed + gathered(m_recv[d])
    inv_rms2 = lax.rsqrt(sq_mixed / model + EPS)
    for copy in u_copies:
        copy.wait()
    for d in range(1, kvn):
        up_sum = up_sum + u_recv[d].astype(f32)
    hidden = jnp.square(jnp.maximum(inv_rms2 * up_sum, 0.0)).astype(bf16)
    h_send[...] = hidden
    h_copies = [remote(h_send, h_recv.at[d], h_sem, (d,), kv_to(d)) for d in range(1, kvn)]
    for copy in h_copies:
        copy.start()

    def down_for(block_of, j):
        span = pl.ds(pl.multiple_of(j * part, part), part)
        return jnp.dot(block_of, dw[span, :], preferred_element_type=f32)

    loads[5].wait()
    down = down_for(hidden, me_kv)
    for d in sorted(range(1, kvn), key=lambda d: min(d, kvn - d)):
        h_copies[d - 1].wait()
        down = down + down_for(h_recv[d], lax.rem(me_kv + kvn - d, kvn))
    for t in range(tpn):
        d_send[t] = down[:, t * width : (t + 1) * width].astype(bf16)
    att_out = [
        remote(d_send.at[lax.rem(me_tp + d, tpn)], d_recv.at[d], d_sem, (d,), tp_to(d))
        for d in range(1, tpn)
    ]
    for copy in att_out:
        copy.start()
    result = jnp.zeros((rows, width), f32)
    for t in range(tpn):
        here = slice(t * width, (t + 1) * width)
        result = jnp.where(me_tp == t, mixed[:, here] + down[:, here], result)
    for copy in att_out:
        copy.wait()
    for d in range(1, tpn):
        result = result + d_recv[d].astype(f32)
    out_ref[...] = result.astype(bf16)


def fused_body(
    kvn,
    tpn,
    residual,
    cache_keys,
    cache_values,
    norm_gain,
    query_weight,
    key_weight,
    value_weight,
    head_lambda,
    head_gain,
    out_weight,
    mixer_gain,
    up_weight,
    down_weight,
):
    f32 = jnp.float32
    bf16 = jnp.bfloat16
    rows, width = residual.shape
    positions, kv_local = cache_keys.shape[1:3]
    depth, q_cols = query_weight.shape
    k_cols = key_weight.shape[1]
    part = up_weight.shape[1] // kvn
    reps = q_cols // VDIM * 2
    groups = 4
    keys = cache_keys.reshape(rows, positions * kv_local, VDIM)
    values = cache_values.reshape(rows, positions * kv_local, VDIM)
    gains = jnp.stack(
        [norm_gain, mixer_gain, jnp.pad(head_gain, (0, depth - VDIM))]
    ).astype(f32)
    vmem = pl.BlockSpec(memory_space=pltpu.VMEM)
    away = pl.BlockSpec(memory_space=pl.ANY)
    big = (keys, values, query_weight, key_weight, value_weight, out_weight, up_weight, down_weight)
    V = pltpu.VMEM
    dma = pltpu.SemaphoreType.DMA
    scratch = [V(a.shape, a.dtype) for a in big] + [
        V((tpn, rows, width), bf16),
        V((rows, q_cols + 128), bf16),
        V((kvn, rows, q_cols + 128), bf16),
        V((rows, 2 * k_cols), bf16),
        V((kvn, rows, 2 * k_cols), bf16),
        V((rows, reps, VDIM), f32),
        V((rows, reps, VDIM), f32),
        V((rows, reps, VDIM), f32),
        V((rows * reps, VDIM), f32),
        V((rows * reps, VDIM), bf16),
        V((kvn, rows * reps, VDIM), bf16),
        V((reps, 128), f32),
        V((kvn, reps, 128), f32),
        V((rows, reps, VDIM), f32),
        V((tpn, rows, depth), bf16),
        V((rows, depth), bf16),
        V((rows, 128), bf16),
        V((kvn, rows, 128), bf16),
        V((kvn, rows, part), bf16),
        V((kvn, rows, part), bf16),
        V((rows, part), bf16),
        V((kvn, rows, part), bf16),
        V((tpn, rows, width), bf16),
        V((tpn, rows, width), bf16),
        dma((6,)),
        dma((groups, 2)),
        dma((2, tpn)),
        dma((2, kvn)),
        dma((2, kvn)),
        dma((2, groups, kvn)),
        dma((2, kvn)),
        dma((2, tpn)),
        dma((2, kvn)),
        dma((2, kvn)),
        dma((2, kvn)),
        dma((2, tpn)),
    ]
    return pl.pallas_call(
        functools.partial(layer_kernel, (kvn, tpn, kv_local, groups)),
        out_shape=jax.ShapeDtypeStruct((rows, width), bf16),
        in_specs=[vmem, vmem, pl.BlockSpec(memory_space=pltpu.SMEM)] + [away] * 8,
        out_specs=vmem,
        scratch_shapes=scratch,
        compiler_params=pltpu.CompilerParams(
            collective_id=0, has_side_effects=True, vmem_limit_bytes=60 * 2**20
        ),
        name="layer",
    )(residual, gains, head_lambda, *big)


def fits(mesh):
    kvn, tpn = mesh.shape["kv"], mesh.shape["tp"]
    heads = HEADS // tpn
    return D // (kvn * tpn) % 128 == 0 and heads * 2 % 8 == 0 and KV_HEADS // tpn > 1


def solution(mesh):
    kvn, tpn = mesh.shape["kv"], mesh.shape["tp"]
    body = functools.partial(fused_body, kvn, tpn) if fits(mesh) else plain_body
    in_specs = (
        P("grp", ("kv", "tp")),
        P("grp", "kv", "tp", None),
        P("grp", "kv", "tp", None),
        P("kv"),
        P("kv", "tp"),
        P("kv", "tp"),
        P("kv", "tp"),
        P("tp"),
        P(),
        P("tp", "kv"),
        P("kv"),
        P("kv", "tp"),
        P("tp", "kv"),
    )
    out_specs = P("grp", ("kv", "tp"))
    return jax.shard_map(body, mesh=mesh, in_specs=in_specs, out_specs=out_specs, check_vma=False)
```

```python
import functools

import jax
import jax.numpy as jnp
from jax import lax
from jax.experimental import pallas as pl
from jax.experimental.pallas import tpu as pltpu
from jax.sharding import PartitionSpec as P

D = 4096
HEADS = 16
KV_HEADS = 8
HALF = 64
VDIM = 128


EPS = 1e-06


def joined(shard, axis, combine):
    everything = jax.tree.map(lambda part: lax.all_gather(part, axis), shard)
    first = jax.tree.map(lambda part: part[0], everything)

    def step(k, so_far):
        return combine(so_far, jax.tree.map(lambda part: part[k], everything))

    return lax.fori_loop(1, lax.axis_size(axis), step, first)


def combine(first, second):
    top = jnp.maximum(first[0], second[0])
    left = jnp.exp(first[0] - top)
    right = jnp.exp(second[0] - top)
    return (
        top,
        first[1] * left + second[1] * right,
        first[2] * left[..., None] + second[2] * right[..., None],
    )


def plain_body(
    residual,
    cache_keys,
    cache_values,
    norm_gain,
    query_weight,
    key_weight,
    value_weight,
    head_lambda,
    head_gain,
    out_weight,
    mixer_gain,
    up_weight,
    down_weight,
):
    f32 = jnp.float32
    bf16 = jnp.bfloat16
    rows = residual.shape[0]
    kv_local = cache_keys.shape[2]
    group = HEADS // KV_HEADS
    scale = 1.0 / HALF**0.5
    block = lax.all_gather(residual, "tp", axis=1, tiled=True).astype(f32)
    scaled = (block * norm_gain.astype(f32)).astype(bf16)
    q_part = jnp.dot(scaled, query_weight, preferred_element_type=f32)
    k_part = jnp.dot(scaled, key_weight, preferred_element_type=f32)
    v_part = jnp.dot(scaled, value_weight, preferred_element_type=f32)
    sq_part = jnp.sum(block * block, axis=1)
    q_sum, k_sum, v_sum, sq_sum = lax.psum((q_part, k_part, v_part, sq_part), "kv")
    inv_rms = lax.rsqrt(sq_sum / D + EPS)[:, None]
    query = (inv_rms * q_sum).astype(bf16).reshape(rows, kv_local, group, 2, HALF)
    new_key = (inv_rms * k_sum).astype(bf16).reshape(rows, kv_local, 2, HALF)
    new_value = (inv_rms * v_sum).astype(bf16).reshape(rows, kv_local, VDIM)
    positions = cache_keys.shape[1]
    keys = cache_keys.reshape(rows, positions, kv_local, 2, HALF)
    scores = jnp.einsum("bkgch,bpkch->bkgcp", query, keys, preferred_element_type=f32) * scale
    local_top = jnp.max(scores, axis=4)
    expo = jnp.exp(scores - local_top[..., None])
    local_total = jnp.sum(expo, axis=4)
    local_weighted = jnp.einsum(
        "bkgcp,bpkv->bkgcv", expo.astype(bf16), cache_values, preferred_element_type=f32
    )
    cache_top, total, weighted = joined((local_top, local_total, local_weighted), "kv", combine)
    own = jnp.einsum("bkgch,bkch->bkgc", query, new_key, preferred_element_type=f32) * scale
    top = jnp.maximum(cache_top, own)
    old_part = jnp.exp(cache_top - top)
    own_part = jnp.exp(own - top)
    numer = (
        weighted * old_part[..., None]
        + own_part[..., None] * new_value.astype(f32)[:, :, None, None, :]
    )
    attended = numer / (total * old_part + own_part)[..., None]
    lambdas = head_lambda.reshape(kv_local, group)[None, :, :, None]
    diff = attended[:, :, :, 0] - lambdas * attended[:, :, :, 1]
    normed = (
        diff * lax.rsqrt(jnp.mean(diff * diff, axis=3, keepdims=True) + EPS) * head_gain.astype(f32)
    )
    heads_out = normed.astype(bf16).reshape(rows, kv_local * group * VDIM)
    projected = jnp.dot(heads_out, out_weight, preferred_element_type=f32)
    mixed = (
        residual.astype(f32) + lax.psum_scatter(projected, "tp", scatter_dimension=1, tiled=True)
    ).astype(bf16)
    mixed_block = lax.all_gather(mixed, "tp", axis=1, tiled=True).astype(f32)
    scaled2 = (mixed_block * mixer_gain.astype(f32)).astype(bf16)
    up_part = jnp.dot(scaled2, up_weight, preferred_element_type=f32)
    sq_mixed = jnp.sum(mixed_block * mixed_block, axis=1)
    up_share = lax.psum_scatter(up_part, "kv", scatter_dimension=1, tiled=True)
    sq_total = lax.psum(sq_mixed, "kv")
    inv_rms2 = lax.rsqrt(sq_total / D + EPS)[:, None]
    share = jnp.square(jnp.maximum(inv_rms2 * up_share, 0.0)).astype(bf16)
    hidden = lax.all_gather(share, "kv", axis=1, tiled=True)
    down_part = jnp.dot(hidden, down_weight, preferred_element_type=f32)
    return (
        mixed.astype(f32) + lax.psum_scatter(down_part, "tp", scatter_dimension=1, tiled=True)
    ).astype(bf16)


def spread(column, lanes):
    high = column.astype(jnp.bfloat16).astype(jnp.float32)
    lane = lax.broadcasted_iota(jnp.int32, (column.shape[0], lanes), 1)
    return jnp.where(lane < lanes // 2, high, column - high).astype(jnp.bfloat16)


def gathered(pair):
    pair = pair.astype(jnp.float32)
    half = pair.shape[1] // 2
    return pair[:, 0:1] + pair[:, half : half + 1]


def partner(index, distance):
    bit = 1
    while bit <= distance:
        if distance & bit:
            index = index + bit - 2 * bit * ((index // bit) % 2)
        bit *= 2
    return index


def layer_kernel(
    dims,
    residual_ref,
    norm_ref,
    mixer_ref,
    head_ref,
    lambda_ref,
    keys_hbm,
    values_hbm,
    qw_hbm,
    kw_hbm,
    vw_hbm,
    ow_hbm,
    uw_hbm,
    dw_hbm,
    out_ref,
    keys,
    values,
    qw,
    kw,
    vw,
    ow,
    uw,
    dw,
    x_all,
    q_send,
    q_recv,
    r_send,
    r_recv,
    n_send,
    n_recv,
    q_rows,
    k_rows,
    v_rows,
    w_own,
    w_send,
    w_recv,
    s_send,
    s_recv,
    att,
    o_all,
    o_send,
    m_send,
    m_recv,
    u_send,
    u_recv,
    h_send,
    h_recv,
    d_send,
    d_recv,
    load_sem,
    cache_sem,
    x_sem,
    q_sem,
    r_sem,
    n_sem,
    w_sem,
    s_sem,
    o_sem,
    m_sem,
    u_sem,
    h_sem,
    d_sem,
):
    f32 = jnp.float32
    bf16 = jnp.bfloat16
    kvn, tpn, kv_local, groups = dims
    rows = residual_ref.shape[0]
    width = residual_ref.shape[1]
    q_cols = qw.shape[1]
    k_cols = kw.shape[1]
    reps = q_cols // VDIM * 2
    per = rows // groups
    model = qw.shape[0] * kvn
    me_kv = lax.axis_index("kv")
    me_tp = lax.axis_index("tp")

    far_kv = list(reversed(range(1, kvn)))
    far_tp = list(reversed(range(1, tpn)))
    loads = []
    for index, (src, dst) in enumerate(((qw_hbm, qw), (kw_hbm, kw), (vw_hbm, vw))):
        loads.append(pltpu.make_async_copy(src, dst, load_sem.at[index]))
        loads[-1].start()

    def cache_copy(g, which):
        src, dst = ((keys_hbm, keys), (values_hbm, values))[which]
        span = pl.ds(g * per, per)
        return pltpu.make_async_copy(src.at[span], dst.at[span], cache_sem.at[g, which])

    for g in range(groups):
        cache_copy(g, 0).start()
        cache_copy(g, 1).start()
    def kv_to(d):
        return {"kv": partner(me_kv, d)}

    def tp_to(d):
        return {"tp": partner(me_tp, d)}

    def remote(src, dst, sems, index, target):
        return pltpu.make_async_remote_copy(
            src_ref=src,
            dst_ref=dst,
            send_sem=sems.at[(0,) + index],
            recv_sem=sems.at[(1,) + index],
            device_id=target,
            device_id_type=pl.DeviceIdType.MESH,
        )

    barrier = pltpu.get_barrier_semaphore()
    for d in range(1, tpn):
        pl.semaphore_signal(barrier, 1, device_id=tp_to(d), device_id_type=pl.DeviceIdType.MESH)
    for d in range(1, kvn):
        pl.semaphore_signal(barrier, 1, device_id=kv_to(d), device_id_type=pl.DeviceIdType.MESH)
    pl.semaphore_wait(barrier, tpn + kvn - 2)

    x_copies = [
        remote(residual_ref, x_all.at[me_tp], x_sem, (d,), tp_to(d)) for d in reversed(range(1, tpn))
    ]
    for copy in x_copies:
        copy.start()
    x_all[me_tp] = residual_ref[...]
    for copy in x_copies:
        copy.wait()
    for index, (src, dst) in enumerate(((ow_hbm, ow), (uw_hbm, uw), (dw_hbm, dw))):
        loads.append(pltpu.make_async_copy(src, dst, load_sem.at[3 + index]))
        loads[-1].start()

    block = jnp.concatenate([x_all[t] for t in range(tpn)], axis=1).astype(f32)
    scaled = (block * norm_ref[...].astype(f32)[None, :]).astype(bf16)
    sq_own = jnp.sum(block * block, axis=1, keepdims=True)
    r_send[...] = spread(sq_own, 128)
    r_copies = [remote(r_send, r_recv.at[d], r_sem, (d,), kv_to(d)) for d in far_kv]
    for copy in r_copies:
        copy.start()
    loads[0].wait()
    q_own = jnp.dot(scaled, qw[...], preferred_element_type=f32)
    q_send[...] = q_own.astype(bf16)
    q_copies = [remote(q_send, q_recv.at[d], q_sem, (d,), kv_to(d)) for d in far_kv]
    for copy in q_copies:
        copy.start()
    loads[1].wait()
    loads[2].wait()
    k_own = jnp.dot(scaled, kw[...], preferred_element_type=f32)
    v_own = jnp.dot(scaled, vw[...], preferred_element_type=f32)
    n_send[:, 0:k_cols] = k_own.astype(bf16)
    n_send[:, k_cols:] = v_own.astype(bf16)
    for copy in r_copies:
        copy.wait()
    for copy in q_copies:
        copy.wait()
    n_copies = [remote(n_send, n_recv.at[d], n_sem, (d,), kv_to(d)) for d in far_kv]
    for copy in n_copies:
        copy.start()
    sq_sum = sq_own
    q_sum = q_own
    for d in range(1, kvn):
        sq_sum = sq_sum + gathered(r_recv[d])
        q_sum = q_sum + q_recv[d].astype(f32)
    inv_rms = lax.rsqrt(sq_sum / model + EPS)
    scale = 1.0 / HALF**0.5
    query = (inv_rms * q_sum).astype(bf16).astype(f32) * scale
    low_half = lax.broadcasted_iota(jnp.int32, (rows, VDIM), 1) < HALF
    for h in range(reps // 2):
        piece = query[:, h * VDIM : (h + 1) * VDIM]
        q_rows[:, 2 * h, :] = jnp.where(low_half, piece, 0.0)
        q_rows[:, 2 * h + 1, :] = jnp.where(low_half, 0.0, piece)

    columns = keys.shape[1]
    share = reps // kv_local
    col = lax.broadcasted_iota(jnp.int32, (2 * reps, columns), 1)
    row = lax.broadcasted_iota(jnp.int32, (2 * reps, columns), 0)
    valid = lax.rem(col, kv_local) == lax.rem(row, reps) // share
    lane = lax.broadcasted_iota(jnp.int32, (reps, 128), 1)

    def w_copy(p, d):
        span = slice(p * 2 * reps, (p + 1) * 2 * reps)
        return remote(w_send.at[span], w_recv.at[d, span], w_sem, (p, d), kv_to(d))

    def scores_of(p):
        b = 2 * p
        none = jnp.zeros((reps, VDIM), f32)
        both = jnp.concatenate(
            [
                jnp.concatenate([q_rows[b], none], axis=1),
                jnp.concatenate([none, q_rows[b + 1]], axis=1),
            ],
            axis=0,
        ).astype(bf16)
        return lax.dot_general(
            both,
            jnp.concatenate([keys[b], keys[b + 1]], axis=1),
            (((1,), (1,)), ((), ())),
            preferred_element_type=f32,
        )

    for g in range(groups):
        cache_copy(g, 0).wait()
        cache_copy(g, 1).wait()
    stat = jnp.zeros((reps, 128), f32)
    pairs = rows // 2
    scores = scores_of(0)
    for p in range(pairs):
        b = 2 * p
        later = scores_of(p + 1) if p + 1 < pairs else None
        scores = jnp.where(valid, scores, -1e30)
        top = jnp.max(scores, axis=1, keepdims=True)
        expo = jnp.exp(scores - top)
        total = jnp.sum(expo, axis=1, keepdims=True)
        product = jnp.dot(
            expo.astype(bf16),
            jnp.concatenate([values[b], values[b + 1]], axis=1),
            preferred_element_type=f32,
        )
        outs = []
        for side in range(2):
            here = slice(side * reps, (side + 1) * reps)
            outs.append(product[here, side * VDIM : (side + 1) * VDIM])
            stat = jnp.where(lane == b + side, top[here], stat)
            stat = jnp.where(lane == b + side + 64, total[here], stat)
        weighted = jnp.concatenate(outs, axis=0)
        span = slice(p * 2 * reps, (p + 1) * 2 * reps)
        w_own[span, :] = weighted
        w_send[span, :] = weighted.astype(bf16)
        for d in far_kv:
            w_copy(p, d).start()
        scores = later

    s_send[...] = stat
    s_copies = [remote(s_send, s_recv.at[d], s_sem, (d,), kv_to(d)) for d in far_kv]
    for copy in s_copies:
        copy.start()

    for copy in n_copies:
        copy.wait()
    k_sum, v_sum = k_own, v_own
    for d in range(1, kvn):
        k_sum = k_sum + n_recv[d, :, 0:k_cols].astype(f32)
        v_sum = v_sum + n_recv[d, :, k_cols:].astype(f32)
    new_key = (inv_rms * k_sum).astype(bf16).astype(f32)
    new_value = (inv_rms * v_sum).astype(bf16).astype(f32)
    for r in range(reps):
        k = r // share
        k_rows[:, r, :] = new_key[:, k * VDIM : (k + 1) * VDIM]
        v_rows[:, r, :] = new_value[:, k * VDIM : (k + 1) * VDIM]
    own = jnp.zeros((reps, 128), f32)
    for b in range(rows):
        own = jnp.where(lane == b, jnp.sum(q_rows[b] * k_rows[b], axis=1, keepdims=True), own)

    for copy in s_copies:
        copy.wait()
    stats = [stat] + [s_recv[d] for d in range(1, kvn)]
    top = own
    for part in stats:
        top = jnp.maximum(top, part)
    own_part = jnp.exp(own - top)
    denom = own_part
    factors = []
    for part in stats:
        factors.append(jnp.exp(part - top))
        denom = denom + factors[-1] * pltpu.roll(part, 64, 1)
    own_part = own_part / denom
    factors = [factor / denom for factor in factors]
    for p in range(pairs):
        for d in far_kv:
            w_copy(p, d).wait()
    for b in range(rows):
        span = slice(b * reps, (b + 1) * reps)
        total = v_rows[b] * own_part[:, b : b + 1] + w_own[span, :] * factors[0][:, b : b + 1]
        for d in range(1, kvn):
            total = total + w_recv[d, span, :].astype(f32) * factors[d][:, b : b + 1]
        att[b] = total

    heads = []
    for h in range(reps // 2):
        diff = att[:, 2 * h, :] - lambda_ref[h] * att[:, 2 * h + 1, :]
        mean = jnp.mean(diff * diff, axis=1, keepdims=True)
        heads.append((diff * lax.rsqrt(mean + EPS) * head_ref[...].astype(f32)[None, :]).astype(bf16))
    heads_out = jnp.concatenate(heads, axis=1)
    loads[3].wait()
    o_send[...] = jnp.dot(heads_out, ow[...], preferred_element_type=f32).astype(bf16)
    o_copies = [remote(o_send, o_all.at[me_tp], o_sem, (d,), tp_to(d)) for d in far_tp]
    for copy in o_copies:
        copy.start()
    o_all[me_tp] = o_send[...]
    for copy in o_copies:
        copy.wait()
    mixed = o_all[0].astype(f32)
    for t in range(1, tpn):
        mixed = mixed + o_all[t].astype(f32)
    mixed = (block + mixed).astype(bf16).astype(f32)
    scaled2 = (mixed * mixer_ref[...].astype(f32)[None, :]).astype(bf16)
    sq_mixed = jnp.sum(mixed * mixed, axis=1, keepdims=True)
    m_send[...] = spread(sq_mixed, 128)
    m_copies = [remote(m_send, m_recv.at[d], m_sem, (d,), kv_to(d)) for d in far_kv]
    for copy in m_copies:
        copy.start()

    part = uw.shape[1] // kvn

    piece = part // 2

    def up_for(j, half):
        span = pl.ds(pl.multiple_of(j * part + half * piece, piece), piece)
        return jnp.dot(scaled2, uw[:, span], preferred_element_type=f32)

    loads[4].wait()
    u_copies = {}
    for half in range(2):
        for d in far_kv:
            u_send[half, d] = up_for(partner(me_kv, d), half).astype(bf16)
            u_copies[half, d] = remote(
                u_send.at[half, d], u_recv.at[half, d], u_sem, (half, d), kv_to(d)
            )
            u_copies[half, d].start()
    up_own = [up_for(me_kv, half) for half in range(2)]
    for copy in m_copies:
        copy.wait()
    for d in range(1, kvn):
        sq_mixed = sq_mixed + gathered(m_recv[d])
    inv_rms2 = lax.rsqrt(sq_mixed / model + EPS)
    h_copies = {}
    own_hidden = []
    for half in range(2):
        for d in far_kv:
            u_copies[half, d].wait()
        up_sum = up_own[half]
        for d in range(1, kvn):
            up_sum = up_sum + u_recv[half, d].astype(f32)
        hidden = jnp.square(jnp.maximum(inv_rms2 * up_sum, 0.0)).astype(bf16)
        own_hidden.append(hidden)
        h_send[half] = hidden
        for d in far_kv:
            h_copies[half, d] = remote(
                h_send.at[half], h_recv.at[half, d], h_sem, (half, d), kv_to(d)
            )
            h_copies[half, d].start()

    def down_for(block_of, j, half):
        span = pl.ds(pl.multiple_of(j * part + half * piece, piece), piece)
        return jnp.dot(block_of, dw[span, :], preferred_element_type=f32)

    loads[5].wait()
    down = down_for(own_hidden[0], me_kv, 0) + down_for(own_hidden[1], me_kv, 1)
    for half in range(2):
        for d in range(1, kvn):
            h_copies[half, d].wait()
            down = down + down_for(h_recv[half, d], partner(me_kv, d), half)
    for t in range(tpn):
        d_send[t] = down[:, t * width : (t + 1) * width].astype(bf16)
    att_out = [
        remote(d_send.at[partner(me_tp, d)], d_recv.at[d], d_sem, (d,), tp_to(d))
        for d in reversed(range(1, tpn))
    ]
    for copy in att_out:
        copy.start()
    result = jnp.zeros((rows, width), f32)
    for t in range(tpn):
        here = slice(t * width, (t + 1) * width)
        result = jnp.where(me_tp == t, mixed[:, here] + down[:, here], result)
    for copy in att_out:
        copy.wait()
    for d in range(1, tpn):
        result = result + d_recv[d].astype(f32)
    out_ref[...] = result.astype(bf16)


def fused_body(
    kvn,
    tpn,
    residual,
    cache_keys,
    cache_values,
    norm_gain,
    query_weight,
    key_weight,
    value_weight,
    head_lambda,
    head_gain,
    out_weight,
    mixer_gain,
    up_weight,
    down_weight,
):
    f32 = jnp.float32
    bf16 = jnp.bfloat16
    rows, width = residual.shape
    positions, kv_local = cache_keys.shape[1:3]
    depth, q_cols = query_weight.shape
    k_cols = key_weight.shape[1]
    part = up_weight.shape[1] // kvn
    reps = q_cols // VDIM * 2
    groups = 4
    keys = cache_keys.reshape(rows, positions * kv_local, VDIM)
    values = cache_values.reshape(rows, positions * kv_local, VDIM)
    vmem = pl.BlockSpec(memory_space=pltpu.VMEM)
    away = pl.BlockSpec(memory_space=pl.ANY)
    big = (keys, values, query_weight, key_weight, value_weight, out_weight, up_weight, down_weight)
    V = pltpu.VMEM
    dma = pltpu.SemaphoreType.DMA
    scratch = [V(a.shape, a.dtype) for a in big] + [
        V((tpn, rows, width), bf16),
        V((rows, q_cols), bf16),
        V((kvn, rows, q_cols), bf16),
        V((rows, 128), bf16),
        V((kvn, rows, 128), bf16),
        V((rows, 2 * k_cols), bf16),
        V((kvn, rows, 2 * k_cols), bf16),
        V((rows, reps, VDIM), f32),
        V((rows, reps, VDIM), f32),
        V((rows, reps, VDIM), f32),
        V((rows * reps, VDIM), f32),
        V((rows * reps, VDIM), bf16),
        V((kvn, rows * reps, VDIM), bf16),
        V((reps, 128), f32),
        V((kvn, reps, 128), f32),
        V((rows, reps, VDIM), f32),
        V((tpn, rows, depth), bf16),
        V((rows, depth), bf16),
        V((rows, 128), bf16),
        V((kvn, rows, 128), bf16),
        V((2, kvn, rows, part // 2), bf16),
        V((2, kvn, rows, part // 2), bf16),
        V((2, rows, part // 2), bf16),
        V((2, kvn, rows, part // 2), bf16),
        V((tpn, rows, width), bf16),
        V((tpn, rows, width), bf16),
        dma((6,)),
        dma((groups, 2)),
        dma((2, tpn)),
        dma((2, kvn)),
        dma((2, kvn)),
        dma((2, kvn)),
        dma((2, rows // 2, kvn)),
        dma((2, kvn)),
        dma((2, tpn)),
        dma((2, kvn)),
        dma((2, 2, kvn)),
        dma((2, 2, kvn)),
        dma((2, tpn)),
    ]
    return pl.pallas_call(
        functools.partial(layer_kernel, (kvn, tpn, kv_local, groups)),
        out_shape=pltpu.VMEM((rows, width), bf16),
        in_specs=[vmem] * 4 + [pl.BlockSpec(memory_space=pltpu.SMEM)] + [away] * 8,
        out_specs=vmem,
        scratch_shapes=scratch,
        compiler_params=pltpu.CompilerParams(
            collective_id=0, has_side_effects=True, vmem_limit_bytes=60 * 2**20
        ),
        name="layer",
    )(residual, norm_gain, mixer_gain, head_gain, head_lambda, *big)


def fits(mesh):
    kvn, tpn = mesh.shape["kv"], mesh.shape["tp"]
    heads = HEADS // tpn
    paired = kvn & (kvn - 1) == 0 and tpn & (tpn - 1) == 0
    return paired and D // (kvn * tpn) % 128 == 0 and heads * 2 % 8 == 0 and KV_HEADS // tpn > 1


def solution(mesh):
    kvn, tpn = mesh.shape["kv"], mesh.shape["tp"]
    body = functools.partial(fused_body, kvn, tpn) if fits(mesh) else plain_body
    in_specs = (
        P("grp", ("kv", "tp")),
        P("grp", "kv", "tp", None),
        P("grp", "kv", "tp", None),
        P("kv"),
        P("kv", "tp"),
        P("kv", "tp"),
        P("kv", "tp"),
        P("tp"),
        P(),
        P("tp", "kv"),
        P("kv"),
        P("kv", "tp"),
        P("tp", "kv"),
    )
    out_specs = P("grp", ("kv", "tp"))
    return jax.shard_map(body, mesh=mesh, in_specs=in_specs, out_specs=out_specs, check_vma=False)
```

```python
import functools

import jax
import jax.numpy as jnp
from jax import lax
from jax.experimental import pallas as pl
from jax.experimental.pallas import tpu as pltpu
from jax.sharding import PartitionSpec as P

D = 4096
HEADS = 16
KV_HEADS = 8
HALF = 64
VDIM = 128


EPS = 1e-06


def joined(shard, axis, combine):
    everything = jax.tree.map(lambda part: lax.all_gather(part, axis), shard)
    first = jax.tree.map(lambda part: part[0], everything)

    def step(k, so_far):
        return combine(so_far, jax.tree.map(lambda part: part[k], everything))

    return lax.fori_loop(1, lax.axis_size(axis), step, first)


def combine(first, second):
    top = jnp.maximum(first[0], second[0])
    left = jnp.exp(first[0] - top)
    right = jnp.exp(second[0] - top)
    return (
        top,
        first[1] * left + second[1] * right,
        first[2] * left[..., None] + second[2] * right[..., None],
    )


def plain_body(
    residual,
    cache_keys,
    cache_values,
    norm_gain,
    query_weight,
    key_weight,
    value_weight,
    head_lambda,
    head_gain,
    out_weight,
    mixer_gain,
    up_weight,
    down_weight,
):
    f32 = jnp.float32
    bf16 = jnp.bfloat16
    rows = residual.shape[0]
    kv_local = cache_keys.shape[2]
    group = HEADS // KV_HEADS
    scale = 1.0 / HALF**0.5
    block = lax.all_gather(residual, "tp", axis=1, tiled=True).astype(f32)
    scaled = (block * norm_gain.astype(f32)).astype(bf16)
    q_part = jnp.dot(scaled, query_weight, preferred_element_type=f32)
    k_part = jnp.dot(scaled, key_weight, preferred_element_type=f32)
    v_part = jnp.dot(scaled, value_weight, preferred_element_type=f32)
    sq_part = jnp.sum(block * block, axis=1)
    q_sum, k_sum, v_sum, sq_sum = lax.psum((q_part, k_part, v_part, sq_part), "kv")
    inv_rms = lax.rsqrt(sq_sum / D + EPS)[:, None]
    query = (inv_rms * q_sum).astype(bf16).reshape(rows, kv_local, group, 2, HALF)
    new_key = (inv_rms * k_sum).astype(bf16).reshape(rows, kv_local, 2, HALF)
    new_value = (inv_rms * v_sum).astype(bf16).reshape(rows, kv_local, VDIM)
    positions = cache_keys.shape[1]
    keys = cache_keys.reshape(rows, positions, kv_local, 2, HALF)
    scores = jnp.einsum("bkgch,bpkch->bkgcp", query, keys, preferred_element_type=f32) * scale
    local_top = jnp.max(scores, axis=4)
    expo = jnp.exp(scores - local_top[..., None])
    local_total = jnp.sum(expo, axis=4)
    local_weighted = jnp.einsum(
        "bkgcp,bpkv->bkgcv", expo.astype(bf16), cache_values, preferred_element_type=f32
    )
    cache_top, total, weighted = joined((local_top, local_total, local_weighted), "kv", combine)
    own = jnp.einsum("bkgch,bkch->bkgc", query, new_key, preferred_element_type=f32) * scale
    top = jnp.maximum(cache_top, own)
    old_part = jnp.exp(cache_top - top)
    own_part = jnp.exp(own - top)
    numer = (
        weighted * old_part[..., None]
        + own_part[..., None] * new_value.astype(f32)[:, :, None, None, :]
    )
    attended = numer / (total * old_part + own_part)[..., None]
    lambdas = head_lambda.reshape(kv_local, group)[None, :, :, None]
    diff = attended[:, :, :, 0] - lambdas * attended[:, :, :, 1]
    normed = (
        diff * lax.rsqrt(jnp.mean(diff * diff, axis=3, keepdims=True) + EPS) * head_gain.astype(f32)
    )
    heads_out = normed.astype(bf16).reshape(rows, kv_local * group * VDIM)
    projected = jnp.dot(heads_out, out_weight, preferred_element_type=f32)
    mixed = (
        residual.astype(f32) + lax.psum_scatter(projected, "tp", scatter_dimension=1, tiled=True)
    ).astype(bf16)
    mixed_block = lax.all_gather(mixed, "tp", axis=1, tiled=True).astype(f32)
    scaled2 = (mixed_block * mixer_gain.astype(f32)).astype(bf16)
    up_part = jnp.dot(scaled2, up_weight, preferred_element_type=f32)
    sq_mixed = jnp.sum(mixed_block * mixed_block, axis=1)
    up_share = lax.psum_scatter(up_part, "kv", scatter_dimension=1, tiled=True)
    sq_total = lax.psum(sq_mixed, "kv")
    inv_rms2 = lax.rsqrt(sq_total / D + EPS)[:, None]
    share = jnp.square(jnp.maximum(inv_rms2 * up_share, 0.0)).astype(bf16)
    hidden = lax.all_gather(share, "kv", axis=1, tiled=True)
    down_part = jnp.dot(hidden, down_weight, preferred_element_type=f32)
    return (
        mixed.astype(f32) + lax.psum_scatter(down_part, "tp", scatter_dimension=1, tiled=True)
    ).astype(bf16)


def spread(column, lanes):
    high = column.astype(jnp.bfloat16).astype(jnp.float32)
    lane = lax.broadcasted_iota(jnp.int32, (column.shape[0], lanes), 1)
    return jnp.where(lane < lanes // 2, high, column - high).astype(jnp.bfloat16)


def gathered(pair):
    pair = pair.astype(jnp.float32)
    half = pair.shape[1] // 2
    return pair[:, 0:1] + pair[:, half : half + 1]


def partner(index, distance):
    bit = 1
    while bit <= distance:
        if distance & bit:
            index = index + bit - 2 * bit * ((index // bit) % 2)
        bit *= 2
    return index


def layer_kernel(
    dims,
    residual_ref,
    norm_hbm,
    mixer_hbm,
    head_hbm,
    lambda_ref,
    keys_hbm,
    values_hbm,
    qw_hbm,
    kw_hbm,
    vw_hbm,
    ow_hbm,
    uw_hbm,
    dw_hbm,
    out_ref,
    norm_ref,
    mixer_ref,
    head_ref,
    keys,
    values,
    qw,
    kw,
    vw,
    ow,
    uw,
    dw,
    x_all,
    q_send,
    q_recv,
    r_send,
    r_recv,
    n_send,
    n_recv,
    q_rows,
    k_rows,
    v_rows,
    w_own,
    w_send,
    w_recv,
    s_send,
    s_recv,
    att,
    o_all,
    o_send,
    m_send,
    m_recv,
    u_send,
    u_recv,
    h_send,
    h_recv,
    d_send,
    d_recv,
    load_sem,
    cache_sem,
    x_sem,
    q_sem,
    r_sem,
    n_sem,
    w_sem,
    s_sem,
    o_sem,
    m_sem,
    u_sem,
    h_sem,
    d_sem,
):
    f32 = jnp.float32
    bf16 = jnp.bfloat16
    kvn, tpn, kv_local, groups = dims
    rows, width = residual_ref.shape
    q_cols = qw.shape[1]
    k_cols = kw.shape[1]
    reps = q_cols // VDIM * 2
    per = rows // groups
    model = qw.shape[0] * kvn
    me_kv = lax.axis_index("kv")
    me_tp = lax.axis_index("tp")

    far_kv = list(reversed(range(1, kvn)))
    far_tp = list(reversed(range(1, tpn)))
    loads = []
    for index, (src, dst) in enumerate(((qw_hbm, qw), (kw_hbm, kw), (vw_hbm, vw))):
        loads.append(pltpu.make_async_copy(src, dst, load_sem.at[index]))
    small = []
    for index, (src, dst) in enumerate(
        (
            (residual_ref, x_all.at[me_tp]),
            (norm_hbm, norm_ref),
            (mixer_hbm, mixer_ref),
            (head_hbm, head_ref),
        )
    ):
        small.append(pltpu.make_async_copy(src, dst, load_sem.at[6 + index]))
    for copy in small + loads:
        copy.start()

    def cache_copy(g, which):
        src, dst = ((keys_hbm, keys), (values_hbm, values))[which]
        span = pl.ds(g * per, per)
        return pltpu.make_async_copy(src.at[span], dst.at[span], cache_sem.at[g, which])

    def kv_to(d):
        return {"kv": partner(me_kv, d)}

    def tp_to(d):
        return {"tp": partner(me_tp, d)}

    def remote(src, dst, sems, index, target):
        return pltpu.make_async_remote_copy(
            src_ref=src,
            dst_ref=dst,
            send_sem=sems.at[(0,) + index],
            recv_sem=sems.at[(1,) + index],
            device_id=target,
            device_id_type=pl.DeviceIdType.MESH,
        )

    barrier = pltpu.get_barrier_semaphore()
    mesh_id = pl.DeviceIdType.MESH
    for d in range(1, tpn):
        pl.semaphore_signal(barrier, 1, device_id=tp_to(d), device_id_type=mesh_id)
    pl.semaphore_wait(barrier, tpn - 1 + me_kv)
    for d in far_kv:
        pl.semaphore_signal(barrier, 1, device_id=kv_to(d), device_id_type=mesh_id)

    x_copies = [
        remote(residual_ref, x_all.at[me_tp], x_sem, (d,), tp_to(d)) for d in reversed(range(1, tpn))
    ]
    for copy in x_copies:
        copy.start()
    for g in range(groups):
        cache_copy(g, 0).start()
        cache_copy(g, 1).start()
    for copy in small:
        copy.wait()
    for copy in x_copies:
        copy.wait()

    @pl.when(me_kv < kvn - 1)
    def _():
        pl.semaphore_wait(barrier, kvn - 1 - me_kv)

    for index, (src, dst) in enumerate(((ow_hbm, ow), (uw_hbm, uw), (dw_hbm, dw))):
        loads.append(pltpu.make_async_copy(src, dst, load_sem.at[3 + index]))
        loads[-1].start()

    block = jnp.concatenate([x_all[t] for t in range(tpn)], axis=1).astype(f32)
    scaled = (block * norm_ref[...].astype(f32)[None, :]).astype(bf16)
    sq_own = jnp.sum(block * block, axis=1, keepdims=True)
    r_send[...] = spread(sq_own, 128)
    r_copies = [remote(r_send, r_recv.at[d], r_sem, (d,), kv_to(d)) for d in far_kv]
    for copy in r_copies:
        copy.start()
    loads[0].wait()
    q_own = jnp.dot(scaled, qw[...], preferred_element_type=f32)
    q_send[...] = q_own.astype(bf16)
    q_copies = [remote(q_send, q_recv.at[d], q_sem, (d,), kv_to(d)) for d in far_kv]
    for copy in q_copies:
        copy.start()
    loads[1].wait()
    loads[2].wait()
    k_own = jnp.dot(scaled, kw[...], preferred_element_type=f32)
    v_own = jnp.dot(scaled, vw[...], preferred_element_type=f32)
    n_send[:, 0:k_cols] = k_own.astype(bf16)
    n_send[:, k_cols:] = v_own.astype(bf16)
    for copy in r_copies:
        copy.wait()
    for copy in q_copies:
        copy.wait()
    n_copies = [remote(n_send, n_recv.at[d], n_sem, (d,), kv_to(d)) for d in far_kv]
    for copy in n_copies:
        copy.start()
    sq_sum = sq_own
    q_sum = q_own
    for d in range(1, kvn):
        sq_sum = sq_sum + gathered(r_recv[d])
        q_sum = q_sum + q_recv[d].astype(f32)
    inv_rms = lax.rsqrt(sq_sum / model + EPS)
    scale = 1.0 / HALF**0.5
    query = (inv_rms * q_sum).astype(bf16).astype(f32) * scale
    low_half = lax.broadcasted_iota(jnp.int32, (rows, VDIM), 1) < HALF
    for h in range(reps // 2):
        piece = query[:, h * VDIM : (h + 1) * VDIM]
        q_rows[:, 2 * h, :] = jnp.where(low_half, piece, 0.0)
        q_rows[:, 2 * h + 1, :] = jnp.where(low_half, 0.0, piece)

    columns = keys.shape[1]
    share = reps // kv_local
    col = lax.broadcasted_iota(jnp.int32, (2 * reps, columns), 1)
    row = lax.broadcasted_iota(jnp.int32, (2 * reps, columns), 0)
    valid = lax.rem(col, kv_local) == lax.rem(row, reps) // share
    lane = lax.broadcasted_iota(jnp.int32, (reps, 128), 1)

    def w_copy(p, d):
        span = slice(p * 2 * reps, (p + 1) * 2 * reps)
        return remote(w_send.at[span], w_recv.at[d, span], w_sem, (p, d), kv_to(d))

    def scores_of(p):
        b = 2 * p
        none = jnp.zeros((reps, VDIM), f32)
        both = jnp.concatenate(
            [
                jnp.concatenate([q_rows[b], none], axis=1),
                jnp.concatenate([none, q_rows[b + 1]], axis=1),
            ],
            axis=0,
        ).astype(bf16)
        return lax.dot_general(
            both,
            jnp.concatenate([keys[b], keys[b + 1]], axis=1),
            (((1,), (1,)), ((), ())),
            preferred_element_type=f32,
        )

    for g in range(groups):
        cache_copy(g, 0).wait()
        cache_copy(g, 1).wait()
    stat = jnp.zeros((reps, 128), f32)
    pairs = rows // 2
    scores = scores_of(0)
    for p in range(pairs):
        b = 2 * p
        later = scores_of(p + 1) if p + 1 < pairs else None
        scores = jnp.where(valid, scores, -1e30)
        top = jnp.max(scores, axis=1, keepdims=True)
        expo = jnp.exp(scores - top)
        total = jnp.sum(expo, axis=1, keepdims=True)
        product = jnp.dot(
            expo.astype(bf16),
            jnp.concatenate([values[b], values[b + 1]], axis=1),
            preferred_element_type=f32,
        )
        outs = []
        for side in range(2):
            here = slice(side * reps, (side + 1) * reps)
            outs.append(product[here, side * VDIM : (side + 1) * VDIM])
            stat = jnp.where(lane == b + side, top[here], stat)
            stat = jnp.where(lane == b + side + 64, total[here], stat)
        weighted = jnp.concatenate(outs, axis=0)
        span = slice(p * 2 * reps, (p + 1) * 2 * reps)
        w_own[span, :] = weighted
        w_send[span, :] = weighted.astype(bf16)
        for d in far_kv:
            w_copy(p, d).start()
        scores = later

    s_send[...] = stat
    s_copies = [remote(s_send, s_recv.at[d], s_sem, (d,), kv_to(d)) for d in far_kv]
    for copy in s_copies:
        copy.start()

    for copy in n_copies:
        copy.wait()
    k_sum, v_sum = k_own, v_own
    for d in range(1, kvn):
        k_sum = k_sum + n_recv[d, :, 0:k_cols].astype(f32)
        v_sum = v_sum + n_recv[d, :, k_cols:].astype(f32)
    new_key = (inv_rms * k_sum).astype(bf16).astype(f32)
    new_value = (inv_rms * v_sum).astype(bf16).astype(f32)
    for r in range(reps):
        k = r // share
        k_rows[:, r, :] = new_key[:, k * VDIM : (k + 1) * VDIM]
        v_rows[:, r, :] = new_value[:, k * VDIM : (k + 1) * VDIM]
    own = jnp.zeros((reps, 128), f32)
    for b in range(rows):
        own = jnp.where(lane == b, jnp.sum(q_rows[b] * k_rows[b], axis=1, keepdims=True), own)

    for copy in s_copies:
        copy.wait()
    stats = [stat] + [s_recv[d] for d in range(1, kvn)]
    top = own
    for part in stats:
        top = jnp.maximum(top, part)
    own_part = jnp.exp(own - top)
    denom = own_part
    factors = []
    for part in stats:
        factors.append(jnp.exp(part - top))
        denom = denom + factors[-1] * pltpu.roll(part, 64, 1)
    own_part = own_part / denom
    factors = [factor / denom for factor in factors]
    for p in range(pairs):
        for d in far_kv:
            w_copy(p, d).wait()
    for b in range(rows):
        span = slice(b * reps, (b + 1) * reps)
        total = v_rows[b] * own_part[:, b : b + 1] + w_own[span, :] * factors[0][:, b : b + 1]
        for d in range(1, kvn):
            total = total + w_recv[d, span, :].astype(f32) * factors[d][:, b : b + 1]
        att[b] = total

    heads = []
    for h in range(reps // 2):
        diff = att[:, 2 * h, :] - lambda_ref[h] * att[:, 2 * h + 1, :]
        mean = jnp.mean(diff * diff, axis=1, keepdims=True)
        heads.append((diff * lax.rsqrt(mean + EPS) * head_ref[...].astype(f32)[None, :]).astype(bf16))
    heads_out = jnp.concatenate(heads, axis=1)
    loads[3].wait()
    o_send[...] = jnp.dot(heads_out, ow[...], preferred_element_type=f32).astype(bf16)
    o_copies = [remote(o_send, o_all.at[me_tp], o_sem, (d,), tp_to(d)) for d in far_tp]
    for copy in o_copies:
        copy.start()
    o_all[me_tp] = o_send[...]
    for copy in o_copies:
        copy.wait()
    mixed = o_all[0].astype(f32)
    for t in range(1, tpn):
        mixed = mixed + o_all[t].astype(f32)
    mixed = (block + mixed).astype(bf16).astype(f32)
    scaled2 = (mixed * mixer_ref[...].astype(f32)[None, :]).astype(bf16)
    sq_mixed = jnp.sum(mixed * mixed, axis=1, keepdims=True)
    m_send[...] = spread(sq_mixed, 128)
    m_copies = [remote(m_send, m_recv.at[d], m_sem, (d,), kv_to(d)) for d in far_kv]
    for copy in m_copies:
        copy.start()

    part = uw.shape[1] // kvn

    piece = part // 2

    def up_for(j, half):
        span = pl.ds(pl.multiple_of(j * part + half * piece, piece), piece)
        return jnp.dot(scaled2, uw[:, span], preferred_element_type=f32)

    loads[4].wait()
    u_copies = {}
    for half in range(2):
        for d in far_kv:
            u_send[half, d] = up_for(partner(me_kv, d), half).astype(bf16)
            u_copies[half, d] = remote(
                u_send.at[half, d], u_recv.at[half, d], u_sem, (half, d), kv_to(d)
            )
            u_copies[half, d].start()
    up_own = [up_for(me_kv, half) for half in range(2)]
    for copy in m_copies:
        copy.wait()
    for d in range(1, kvn):
        sq_mixed = sq_mixed + gathered(m_recv[d])
    inv_rms2 = lax.rsqrt(sq_mixed / model + EPS)
    h_copies = {}
    own_hidden = []
    for half in range(2):
        for d in far_kv:
            u_copies[half, d].wait()
        up_sum = up_own[half]
        for d in range(1, kvn):
            up_sum = up_sum + u_recv[half, d].astype(f32)
        hidden = jnp.square(jnp.maximum(inv_rms2 * up_sum, 0.0)).astype(bf16)
        own_hidden.append(hidden)
        h_send[half] = hidden
        for d in far_kv:
            h_copies[half, d] = remote(
                h_send.at[half], h_recv.at[half, d], h_sem, (half, d), kv_to(d)
            )
            h_copies[half, d].start()

    def down_for(block_of, j, half):
        span = pl.ds(pl.multiple_of(j * part + half * piece, piece), piece)
        return jnp.dot(block_of, dw[span, :], preferred_element_type=f32)

    loads[5].wait()
    down = down_for(own_hidden[0], me_kv, 0) + down_for(own_hidden[1], me_kv, 1)
    for half in range(2):
        for d in range(1, kvn):
            h_copies[half, d].wait()
            down = down + down_for(h_recv[half, d], partner(me_kv, d), half)
    for t in range(tpn):
        d_send[t] = down[:, t * width : (t + 1) * width].astype(bf16)
    att_out = [
        remote(d_send.at[partner(me_tp, d)], d_recv.at[d], d_sem, (d,), tp_to(d))
        for d in reversed(range(1, tpn))
    ]
    for copy in att_out:
        copy.start()
    result = jnp.zeros((rows, width), f32)
    for t in range(tpn):
        here = slice(t * width, (t + 1) * width)
        result = jnp.where(me_tp == t, mixed[:, here] + down[:, here], result)
    for copy in att_out:
        copy.wait()
    for d in range(1, tpn):
        result = result + d_recv[d].astype(f32)
    out_ref[...] = result.astype(bf16)


def fused_body(
    kvn,
    tpn,
    residual,
    cache_keys,
    cache_values,
    norm_gain,
    query_weight,
    key_weight,
    value_weight,
    head_lambda,
    head_gain,
    out_weight,
    mixer_gain,
    up_weight,
    down_weight,
):
    f32 = jnp.float32
    bf16 = jnp.bfloat16
    rows, width = residual.shape
    positions, kv_local = cache_keys.shape[1:3]
    depth, q_cols = query_weight.shape
    k_cols = key_weight.shape[1]
    part = up_weight.shape[1] // kvn
    reps = q_cols // VDIM * 2
    groups = 4
    keys = cache_keys.reshape(rows, positions * kv_local, VDIM)
    values = cache_values.reshape(rows, positions * kv_local, VDIM)
    vmem = pl.BlockSpec(memory_space=pltpu.VMEM)
    away = pl.BlockSpec(memory_space=pl.ANY)
    big = (keys, values, query_weight, key_weight, value_weight, out_weight, up_weight, down_weight)
    V = pltpu.VMEM
    dma = pltpu.SemaphoreType.DMA
    scratch = [V(a.shape, a.dtype) for a in (norm_gain, mixer_gain, head_gain) + big] + [
        V((tpn, rows, width), bf16),
        V((rows, q_cols), bf16),
        V((kvn, rows, q_cols), bf16),
        V((rows, 128), bf16),
        V((kvn, rows, 128), bf16),
        V((rows, 2 * k_cols), bf16),
        V((kvn, rows, 2 * k_cols), bf16),
        V((rows, reps, VDIM), f32),
        V((rows, reps, VDIM), f32),
        V((rows, reps, VDIM), f32),
        V((rows * reps, VDIM), f32),
        V((rows * reps, VDIM), bf16),
        V((kvn, rows * reps, VDIM), bf16),
        V((reps, 128), f32),
        V((kvn, reps, 128), f32),
        V((rows, reps, VDIM), f32),
        V((tpn, rows, depth), bf16),
        V((rows, depth), bf16),
        V((rows, 128), bf16),
        V((kvn, rows, 128), bf16),
        V((2, kvn, rows, part // 2), bf16),
        V((2, kvn, rows, part // 2), bf16),
        V((2, rows, part // 2), bf16),
        V((2, kvn, rows, part // 2), bf16),
        V((tpn, rows, width), bf16),
        V((tpn, rows, width), bf16),
        dma((10,)),
        dma((groups, 2)),
        dma((2, tpn)),
        dma((2, kvn)),
        dma((2, kvn)),
        dma((2, kvn)),
        dma((2, rows // 2, kvn)),
        dma((2, kvn)),
        dma((2, tpn)),
        dma((2, kvn)),
        dma((2, 2, kvn)),
        dma((2, 2, kvn)),
        dma((2, tpn)),
    ]
    return pl.pallas_call(
        functools.partial(layer_kernel, (kvn, tpn, kv_local, groups)),
        out_shape=pltpu.VMEM((rows, width), bf16),
        in_specs=[away] * 4 + [pl.BlockSpec(memory_space=pltpu.SMEM)] + [away] * 8,
        out_specs=vmem,
        scratch_shapes=scratch,
        compiler_params=pltpu.CompilerParams(
            collective_id=0, has_side_effects=True, vmem_limit_bytes=60 * 2**20
        ),
        name="layer",
    )(residual, norm_gain, mixer_gain, head_gain, head_lambda, *big)


def fits(mesh):
    kvn, tpn = mesh.shape["kv"], mesh.shape["tp"]
    heads = HEADS // tpn
    paired = kvn & (kvn - 1) == 0 and tpn & (tpn - 1) == 0
    return paired and D // (kvn * tpn) % 128 == 0 and heads * 2 % 8 == 0 and KV_HEADS // tpn > 1


def solution(mesh):
    kvn, tpn = mesh.shape["kv"], mesh.shape["tp"]
    body = functools.partial(fused_body, kvn, tpn) if fits(mesh) else plain_body
    in_specs = (
        P("grp", ("kv", "tp")),
        P("grp", "kv", "tp", None),
        P("grp", "kv", "tp", None),
        P("kv"),
        P("kv", "tp"),
        P("kv", "tp"),
        P("kv", "tp"),
        P("tp"),
        P(),
        P("tp", "kv"),
        P("kv"),
        P("kv", "tp"),
        P("tp", "kv"),
    )
    out_specs = P("grp", ("kv", "tp"))
    return jax.shard_map(body, mesh=mesh, in_specs=in_specs, out_specs=out_specs, check_vma=False)
```
